32 devices in a mesh: sp: 8 (over z, y), dp: 4 (over x, core).
Axes of the slice: x: 2, y: 2, z: 4, core: 2. Of those that a mesh axis runs over, the one named last changes fastest.
Arguments:
- queries: bfloat16 [16, 16, 512, 128], P('dp', None, 'sp'), may hold values from -6 to 6
- key_maps: bfloat16 [16, 16, 512, 128], P('dp', None, 'sp'), may hold values from -6 to 6
- value_rows: bfloat16 [16, 16, 512, 128], P('dp', None, 'sp'), may hold values from -6 to 6
- gate_logits: bfloat16 [512, 16, 2048], P('sp', 'dp'), may hold values from -6 to 6
- mix_lambda: float32 [16], replicated, may hold values from 0.3 to 0.8
- head_gain: float32 [128], replicated, may hold values from 0.1 to 1.9
- out_weight: bfloat16 [2048, 2048], P('sp', 'dp'), may hold values from -0.125 to 0.125
Outputs:
- projected: bfloat16 [512, 16, 2048], P('sp', 'dp')
The draws below stay inside these ranges and needn't reach their ends.
All inputs are finite; a program needn't handle non-finite values.
Results may differ from the reference program's by a relative error of at most 0.0075.
Values may be sent and summed in bfloat16 or wider, within the bound.
A program may use at most 64 MiB of HBM per device.

```python
from functools import partial
import jax
import jax.numpy as jnp
from jax import lax

HEADS = 16
HEAD_DIM = 64
V_DIM = 128
STRETCH = 64
BLOCK = 512
D = 2048
LENGTH = 512
BATCH = 16


def draw_pair(key):
    shape = (BATCH, HEADS, LENGTH, 2 * HEAD_DIM)
    query_key = jax.random.fold_in(key, 11)
    keymap_key = jax.random.fold_in(key, 12)
    query_vals = jnp.clip(1.3 * jax.random.normal(query_key, shape, jnp.float32), -6.0, 6.0)
    keymap_vals = jnp.clip(1.3 * jax.random.normal(keymap_key, shape, jnp.float32), -6.0, 6.0)
    return (query_vals, keymap_vals)


def draw_queries(key, part):
    return draw_pair(key)[0].astype(jnp.bfloat16)


def draw_key_maps(key, part):
    return draw_pair(key)[1].astype(jnp.bfloat16)


def levels(stream_key, extent, shards, smallest, largest):
    factor_of, own = 1.0, jax.random.fold_in(stream_key, 6)
    for position, parts in shards:
        draws = jnp.exp(jax.random.uniform(jax.random.fold_in(own, position), (parts,), jnp.float32, smallest / len(shards), largest / len(shards)))
        factor_of = factor_of * jnp.repeat(draws, extent[position] // parts).reshape([-1 if axis == position else 1 for axis in range(len(extent))])
    return factor_of


def scatter_about(stream_key, shape, spread, reach, pieces=(), dtype=jnp.bfloat16):
    entries = spread * jax.random.normal(stream_key, shape, jnp.float32)
    if pieces:
        entries = entries * levels(stream_key, shape, pieces, -0.22, 0.18)
    return jnp.clip(entries, -reach, reach).astype(dtype)


def setup_inputs(seed: int = 0) -> dict:
    key_of = jax.random.split(jax.random.key(seed), 8)
    queries = draw_queries(jax.random.fold_in(key_of[7], 71), 0)
    key_maps = draw_key_maps(jax.random.fold_in(key_of[7], 71), 0)
    value_rows = scatter_about(key_of[2], (BATCH, HEADS, LENGTH, V_DIM), 1.0, 6.0, ((0, 4), (2, 8)))
    gate_logits = scatter_about(key_of[3], (LENGTH, BATCH, D), 1.0, 6.0, ((0, 8), (1, 4)))
    mix_lambda = jnp.clip(jax.random.uniform(key_of[4], (HEADS,), jnp.float32, 0.3, 0.8), 0.3, 0.8)
    head_gain = jnp.clip(1.0 + 0.18 * jax.random.normal(key_of[5], (V_DIM,), jnp.float32), 0.1, 1.9)
    out_weight = scatter_about(key_of[6], (D, D), D ** -0.5, 0.125, ((0, 8), (1, 4)))
    return dict(queries=queries, key_maps=key_maps, value_rows=value_rows, gate_logits=gate_logits, mix_lambda=mix_lambda, head_gain=head_gain, out_weight=out_weight)


def attend_item(operands, segment_ids, head_gain):
    query_item, key_item, value_item, weight_two = operands
    block_len = min(BLOCK, LENGTH)
    score_scale = HEAD_DIM ** (-0.5)
    outputs = []
    for block_index in range(LENGTH // block_len):
        offset = block_index * block_len
        limit = offset + block_len
        query_rows = query_item[offset:limit]
        key_block = key_item[:limit]
        value_block = value_item[:limit]
        visible = segment_ids[None, :limit] <= segment_ids[offset:limit, None]
        mapped = []
        for which in range(2):
            column_span = slice(which * HEAD_DIM, (which + 1) * HEAD_DIM)
            scores = jnp.dot(query_rows[:, column_span], key_block[:, column_span].T, preferred_element_type=jnp.float32) * score_scale
            scores = jnp.where(visible, scores, -1e+30)
            weights = jnp.exp(scores - lax.optimization_barrier(jnp.max(scores, axis=1, keepdims=True)))
            summed = lax.optimization_barrier(jnp.sum(weights, axis=1, keepdims=True))
            product = jnp.dot(weights.astype(jnp.bfloat16), value_block, preferred_element_type=jnp.float32)
            mapped.append(product / summed)
        combined = mapped[0] - weight_two * mapped[1]
        mean_sq = lax.optimization_barrier(jnp.mean(combined * combined, axis=1, keepdims=True))
        outputs.append((combined * lax.rsqrt(mean_sq + 1e-05) * head_gain).astype(jnp.bfloat16))
    return jnp.concatenate(outputs, axis=0)

def reference(queries, key_maps, value_rows, gate_logits, mix_lambda, head_gain, out_weight):
    item_count = BATCH * HEADS
    segment_ids = (jnp.arange(LENGTH) // STRETCH).astype(jnp.int32)
    lambda_items = jnp.tile(mix_lambda, BATCH)
    normed = lax.map(partial(attend_item, segment_ids=segment_ids, head_gain=head_gain), (queries.reshape(item_count, LENGTH, 2 * HEAD_DIM), key_maps.reshape(item_count, LENGTH, 2 * HEAD_DIM), value_rows.reshape(item_count, LENGTH, V_DIM), lambda_items))
    by_token = jnp.transpose(normed.reshape(BATCH, HEADS, LENGTH, V_DIM), (2, 0, 1, 3)).reshape(LENGTH, BATCH, D)
    gated = (jax.nn.sigmoid(gate_logits.astype(jnp.float32)) * by_token.astype(jnp.float32)).astype(jnp.bfloat16)
    output = jnp.dot(gated.reshape(LENGTH * BATCH, D), out_weight, preferred_element_type=jnp.float32)
    return output.astype(jnp.bfloat16).reshape(LENGTH, BATCH, D)
```

```python
import functools

import jax
import jax.numpy as jnp
from jax import lax
from jax.experimental import pallas as pl
from jax.experimental.pallas import tpu as pltpu
from jax.sharding import PartitionSpec as P

HEAD_DIM = 64
STRETCH = 64
LOG2E = 1.4426950408889634


def attend_item(q, k, v, weight_two, gain, store):
    length, cols = q.shape
    block = min(2 * STRETCH, length)
    factor = HEAD_DIM ** (-0.5) * LOG2E
    first_map = lax.broadcasted_iota(jnp.int32, (block, cols), 1) < cols // 2
    row_seg = (lax.broadcasted_iota(jnp.int32, (2 * block, block), 0) % block) // STRETCH
    col_seg = lax.broadcasted_iota(jnp.int32, (2 * block, block), 1) // STRETCH
    visible = col_seg <= row_seg
    for lo in range(0, length, block):
        hi = lo + block
        rows = q[lo:hi]
        zero = jnp.zeros_like(rows)
        both = jnp.concatenate([jnp.where(first_map, rows, zero), jnp.where(first_map, zero, rows)], axis=0)
        scores = lax.dot_general(
            both, k[:hi], (((1,), (1,)), ((), ())), preferred_element_type=jnp.float32
        )
        diag = jnp.where(visible, scores[:, lo:], -1e30)
        scores = jnp.concatenate([scores[:, :lo], diag], axis=1) if lo else diag
        highest = jnp.max(scores, axis=1, keepdims=True)
        weights = jnp.exp2((scores - highest) * factor)
        summed = jnp.sum(weights, axis=1, keepdims=True)
        mapped = (
            jnp.dot(weights.astype(jnp.bfloat16), v[:hi], preferred_element_type=jnp.float32) / summed
        )
        combined = mapped[:block] - weight_two * mapped[block:]
        mean_sq = jnp.mean(combined * combined, axis=1, keepdims=True)
        store(lo, (combined * lax.rsqrt(mean_sq + 1e-05) * gain).astype(jnp.bfloat16))


def exchange_kernel(n, heads, q_ref, k_ref, v_ref, lam_ref, gain_ref, ret_ref, recv, staged, send_sem, recv_sem, back_sem, ret_sem):
    me = lax.axis_index("sp")
    items, toks, cols = q_ref.shape
    per_dev = items // n
    length = n * toks

    barrier = pltpu.get_barrier_semaphore()

    def greet(step, carry):
        pl.semaphore_signal(barrier, inc=1, device_id={"sp": lax.rem(me + step, n)})
        return carry

    lax.fori_loop(1, n, greet, 0)
    pl.semaphore_wait(barrier, n - 1)

    def send_item(j, carry):
        for which, ref in enumerate((q_ref, k_ref, v_ref)):
            pltpu.make_async_copy(
                ref.at[me * per_dev + j], recv.at[j, which, me], recv_sem.at[j]
            ).start()

        def to_peer(step, carry):
            peer = lax.rem(me + step, n)
            for which, ref in enumerate((q_ref, k_ref, v_ref)):
                pltpu.make_async_remote_copy(
                    src_ref=ref.at[peer * per_dev + j],
                    dst_ref=recv.at[j, which, me],
                    send_sem=send_sem.at[j],
                    recv_sem=recv_sem.at[j],
                    device_id={"sp": peer},
                ).start()
            return carry

        return lax.fori_loop(1, n, to_peer, carry)

    lax.fori_loop(0, per_dev, send_item, 0)

    gain = gain_ref[...]

    def work_item(j, carry):
        pltpu.make_async_copy(recv.at[j], recv.at[j], recv_sem.at[j]).wait()
        q = recv[j, 0].reshape(length, cols)
        k = recv[j, 1].reshape(length, cols)
        v = recv[j, 2].reshape(length, cols)
        item = me * per_dev + j

        def store(lo, rows):
            for r in range(0, rows.shape[0], toks):
                staged[j, (lo + r) // toks] = rows[r : r + toks]

        attend_item(q, k, v, lam_ref[lax.rem(item, heads)], gain, store)
        pltpu.make_async_copy(staged.at[j, me], ret_ref.at[item], ret_sem).start()

        def to_peer(step, carry):
            peer = lax.rem(me + step, n)
            pltpu.make_async_remote_copy(
                src_ref=staged.at[j, peer],
                dst_ref=ret_ref.at[item],
                send_sem=back_sem,
                recv_sem=ret_sem,
                device_id={"sp": peer},
            ).start()
            return carry

        return lax.fori_loop(1, n, to_peer, carry)

    lax.fori_loop(0, per_dev, work_item, 0)
    pltpu.make_async_copy(ret_ref, ret_ref, ret_sem).wait()
    others = staged.at[:, pl.ds(0, n - 1)]
    pltpu.make_async_copy(others, others, back_sem).wait()

    def drain(j, carry):
        for which in range(3):
            part = recv.at[j, which, pl.ds(0, n - 1)]
            pltpu.make_async_copy(part, part, send_sem.at[j]).wait()
        return carry

    lax.fori_loop(0, per_dev, drain, 0)


def on_device(n, queries, key_maps, value_rows, gate_logits, mix_lambda, head_gain, out_weight):
    seqs, heads, toks, cols = queries.shape
    items = seqs * heads
    per_dev = items // n
    width = gate_logits.shape[2]
    anywhere = pl.BlockSpec(memory_space=pl.ANY)
    in_vmem = pl.BlockSpec(memory_space=pltpu.VMEM)
    returned = pl.pallas_call(
        functools.partial(exchange_kernel, n, heads),
        out_shape=jax.ShapeDtypeStruct((items, toks, cols), jnp.bfloat16),
        in_specs=[anywhere, anywhere, anywhere, pl.BlockSpec(memory_space=pltpu.SMEM), in_vmem],
        out_specs=in_vmem,
        scratch_shapes=[
            pltpu.VMEM((per_dev, 3, n, toks, cols), jnp.bfloat16),
            pltpu.VMEM((per_dev, n, toks, cols), jnp.bfloat16),
            pltpu.SemaphoreType.DMA((per_dev,)),
            pltpu.SemaphoreType.DMA((per_dev,)),
            pltpu.SemaphoreType.DMA,
            pltpu.SemaphoreType.DMA,
        ],
        compiler_params=pltpu.CompilerParams(
            collective_id=0, has_side_effects=True, vmem_limit_bytes=40 * 2**20
        ),
        cost_estimate=pl.CostEstimate(flops=5 * 10**10, bytes_accessed=2**28, transcendentals=0),
    )(
        queries.reshape(items, toks, cols),
        key_maps.reshape(items, toks, cols),
        value_rows.reshape(items, toks, cols),
        mix_lambda,
        head_gain.reshape(1, cols),
    )
    by_token = jnp.transpose(returned.reshape(seqs, heads, toks, cols), (2, 0, 1, 3)).reshape(
        toks, seqs, width
    )
    gated = (jax.nn.sigmoid(gate_logits.astype(jnp.float32)) * by_token.astype(jnp.float32)).astype(
        jnp.bfloat16
    )
    gathered = lax.all_gather(out_weight, "sp", axis=0, tiled=True)
    result = jnp.dot(
        gated.reshape(toks * seqs, width),
        lax.all_gather(gathered, "dp", axis=1, tiled=True),
        preferred_element_type=jnp.float32,
    )
    return result.astype(jnp.bfloat16).reshape(toks, seqs, width)


def solution(mesh):
    placed = (
        P("dp", None, "sp", None),
        P("dp", None, "sp", None),
        P("dp", None, "sp", None),
        P("sp", "dp", None),
        P(),
        P(),
        P("sp", "dp"),
    )
    return jax.shard_map(
        functools.partial(on_device, mesh.shape["sp"]),
        mesh=mesh,
        in_specs=placed,
        out_specs=P("sp", "dp", None),
        check_vma=False,
    )
```

```python
import functools

import jax
import jax.numpy as jnp
from jax import lax
from jax.experimental import pallas as pl
from jax.experimental.pallas import tpu as pltpu
from jax.sharding import PartitionSpec as P

HEAD_DIM = 64
STRETCH = 64
LOG2E = 1.4426950408889634


def attend_item(q, k, v, weight_two, gain, store):
    length, cols = q.shape
    block = min(2 * STRETCH, length)
    factor = HEAD_DIM ** (-0.5) * LOG2E
    first_map = lax.broadcasted_iota(jnp.int32, (block, cols), 1) < cols // 2
    row_seg = (lax.broadcasted_iota(jnp.int32, (2 * block, block), 0) % block) // STRETCH
    col_seg = lax.broadcasted_iota(jnp.int32, (2 * block, block), 1) // STRETCH
    visible = col_seg <= row_seg
    for lo in range(0, length, block):
        hi = lo + block
        rows = q[lo:hi]
        zero = jnp.zeros_like(rows)
        both = jnp.concatenate([jnp.where(first_map, rows, zero), jnp.where(first_map, zero, rows)], axis=0)
        scores = lax.dot_general(
            both, k[:hi], (((1,), (1,)), ((), ())), preferred_element_type=jnp.float32
        )
        diag = jnp.where(visible, scores[:, lo:], -1e30)
        scores = jnp.concatenate([scores[:, :lo], diag], axis=1) if lo else diag
        highest = jnp.max(scores, axis=1, keepdims=True)
        weights = jnp.exp2((scores - highest) * factor)
        summed = jnp.sum(weights, axis=1, keepdims=True)
        mapped = (
            jnp.dot(weights.astype(jnp.bfloat16), v[:hi], preferred_element_type=jnp.float32) / summed
        )
        combined = mapped[:block] - weight_two * mapped[block:]
        mean_sq = jnp.mean(combined * combined, axis=1, keepdims=True)
        store(lo, (combined * lax.rsqrt(mean_sq + 1e-05) * gain).astype(jnp.bfloat16))


def exchange_kernel(n, heads, q_ref, k_ref, v_ref, lam_ref, gain_ref, ret_ref, recv, staged, send_sem, recv_sem, back_sem, ret_sem):
    me = lax.axis_index("sp")
    items, toks, cols = q_ref.shape
    per_dev = items // n
    length = n * toks

    barrier = pltpu.get_barrier_semaphore()

    def greet(step, carry):
        pl.semaphore_signal(barrier, inc=1, device_id={"sp": lax.rem(me + step, n)})
        return carry

    lax.fori_loop(1, n, greet, 0)
    pl.semaphore_wait(barrier, n - 1)

    def send_item(j, carry):
        for which, ref in enumerate((q_ref, k_ref, v_ref)):
            pltpu.make_async_copy(
                ref.at[me * per_dev + j], recv.at[j, which, me], recv_sem.at[j]
            ).start()

        def to_peer(step, carry):
            peer = lax.rem(me + step, n)
            for which, ref in enumerate((q_ref, k_ref, v_ref)):
                pltpu.make_async_remote_copy(
                    src_ref=ref.at[peer * per_dev + j],
                    dst_ref=recv.at[j, which, me],
                    send_sem=send_sem.at[j],
                    recv_sem=recv_sem.at[j],
                    device_id={"sp": peer},
                ).start()
            return carry

        return lax.fori_loop(1, n, to_peer, carry)

    lax.fori_loop(0, per_dev, send_item, 0)

    gain = gain_ref[...]

    def work_item(j, carry):
        pltpu.make_async_copy(recv.at[j], recv.at[j], recv_sem.at[j]).wait()
        q = recv[j, 0].reshape(length, cols)
        k = recv[j, 1].reshape(length, cols)
        v = recv[j, 2].reshape(length, cols)
        item = me * per_dev + j

        def store(lo, rows):
            for r in range(0, rows.shape[0], toks):
                staged[j, (lo + r) // toks] = rows[r : r + toks]

        attend_item(q, k, v, lam_ref[lax.rem(item, heads)], gain, store)
        pltpu.make_async_copy(staged.at[j, me], ret_ref.at[item], ret_sem).start()

        def to_peer(step, carry):
            peer = lax.rem(me + step, n)
            pltpu.make_async_remote_copy(
                src_ref=staged.at[j, peer],
                dst_ref=ret_ref.at[item],
                send_sem=back_sem,
                recv_sem=ret_sem,
                device_id={"sp": peer},
            ).start()
            return carry

        return lax.fori_loop(1, n, to_peer, carry)

    lax.fori_loop(0, per_dev, work_item, 0)
    pltpu.make_async_copy(ret_ref, ret_ref, ret_sem).wait()
    others = staged.at[:, pl.ds(0, n - 1)]
    pltpu.make_async_copy(others, others, back_sem).wait()

    def drain(j, carry):
        for which in range(3):
            part = recv.at[j, which, pl.ds(0, n - 1)]
            pltpu.make_async_copy(part, part, send_sem.at[j]).wait()
        return carry

    lax.fori_loop(0, per_dev, drain, 0)


def on_device(n, queries, key_maps, value_rows, gate_logits, mix_lambda, head_gain, out_weight):
    seqs, heads, toks, cols = queries.shape
    items = seqs * heads
    per_dev = items // n
    width = gate_logits.shape[2]
    anywhere = pl.BlockSpec(memory_space=pl.ANY)
    in_vmem = pl.BlockSpec(memory_space=pltpu.VMEM)
    returned = pl.pallas_call(
        functools.partial(exchange_kernel, n, heads),
        out_shape=jax.ShapeDtypeStruct((items, toks, cols), jnp.bfloat16),
        in_specs=[anywhere, anywhere, anywhere, pl.BlockSpec(memory_space=pltpu.SMEM), in_vmem],
        out_specs=in_vmem,
        scratch_shapes=[
            pltpu.VMEM((per_dev, 3, n, toks, cols), jnp.bfloat16),
            pltpu.VMEM((per_dev, n, toks, cols), jnp.bfloat16),
            pltpu.SemaphoreType.DMA((per_dev,)),
            pltpu.SemaphoreType.DMA((per_dev,)),
            pltpu.SemaphoreType.DMA,
            pltpu.SemaphoreType.DMA,
        ],
        compiler_params=pltpu.CompilerParams(
            collective_id=0, has_side_effects=True, vmem_limit_bytes=40 * 2**20
        ),
        cost_estimate=pl.CostEstimate(flops=5 * 10**10, bytes_accessed=2**28, transcendentals=0),
    )(
        queries.reshape(items, toks, cols),
        key_maps.reshape(items, toks, cols),
        value_rows.reshape(items, toks, cols),
        mix_lambda,
        head_gain.reshape(1, cols),
    )
    by_token = jnp.transpose(returned.reshape(seqs, heads, toks, cols), (2, 0, 1, 3)).reshape(
        toks, seqs, width
    )
    gated = (jax.nn.sigmoid(gate_logits.astype(jnp.float32)) * by_token.astype(jnp.float32)).astype(
        jnp.bfloat16
    )
    gathered = lax.all_gather(out_weight, ("dp", "sp"), axis=0, tiled=True)
    result = jnp.einsum(
        "tk,ckn->tcn",
        gated.reshape(toks * seqs, width),
        gathered.reshape(-1, width, out_weight.shape[1]),
        preferred_element_type=jnp.float32,
    )
    return result.astype(jnp.bfloat16).reshape(toks, seqs, width)


def solution(mesh):
    placed = (
        P("dp", None, "sp", None),
        P("dp", None, "sp", None),
        P("dp", None, "sp", None),
        P("sp", "dp", None),
        P(),
        P(),
        P("sp", "dp"),
    )
    return jax.shard_map(
        functools.partial(on_device, mesh.shape["sp"]),
        mesh=mesh,
        in_specs=placed,
        out_specs=P("sp", "dp", None),
        check_vma=False,
    )
```
